32 devices in a mesh: ep: 4 (over y, x), tp: 8 (over z, core).
Axes of the slice: x: 2, y: 2, z: 4, core: 2. Of those that a mesh axis runs over, the one named last changes fastest.
Arguments:
- tokens: bfloat16 [64, 2048], P('ep', 'tp'), may hold values from -6 to 6
- key_cache: bfloat16 [64, 16, 1024, 128], P('ep', 'tp'), may hold values from -1700 to 1700
- value_cache: bfloat16 [64, 16, 1024, 128], P('ep', 'tp'), may hold values from -6 to 6
- gate_totals: float32 [64, 16, 1024], P('ep', 'tp'), as said below
- lengths: int32 [64], P('ep'), may hold values from 128 to 1024
- attn_gain: float32 [2048], replicated, may hold values from 0.1 to 1.9
- w_query: bfloat16 [2048, 2048], P(None, 'tp'), may hold values from -0.125 to 0.125
- w_key: bfloat16 [2048, 2048], P(None, 'tp'), may hold values from -0.125 to 0.125
- w_value: bfloat16 [2048, 2048], P(None, 'tp'), may hold values from -0.125 to 0.125
- w_forget: bfloat16 [2048, 16], replicated, may hold values from -0.125 to 0.125
- forget_bias: float32 [16], replicated, may hold values from -3 to 0
- w_attn_out: bfloat16 [2048, 2048], P('tp'), may hold values from -0.1875 to 0.1875
- moe_gain: float32 [2048], replicated, may hold values from 0.1 to 1.9
- group_ids: int32 [64, 1], P('ep'), may hold values from 0 to 3; in each aligned block of 16 rows (0 to 15, 16 to 31, ...) at most 8 rows name the same one
- inner_ids: int32 [64, 2], P('ep'), may hold values from 0 to 3, all different within a row
- group_prob: float32 [64], P('ep'), may hold values from 0.2 to 1
- pair_logits: float32 [64, 2], P('ep'), may hold values from -6 to 6
- w_expert_gate: bfloat16 [4, 2048, 2048], P('ep', None, 'tp'), may hold values from -0.125 to 0.125
- w_expert_up: bfloat16 [4, 2048, 2048], P('ep', None, 'tp'), may hold values from -0.125 to 0.125
- w_expert_down: bfloat16 [4, 2048, 2048], P('ep', 'tp'), may hold values from -0.375 to 0.375
- w_dense_in: bfloat16 [2048, 2048], P(None, 'tp'), may hold values from -0.125 to 0.125
- w_dense_out: bfloat16 [2048, 2048], P('tp'), may hold values from -0.1875 to 0.1875
- dense_gate: float32 [2048], P('tp'), may hold values from -2 to 2
Outputs:
- layer_output: bfloat16 [64, 2048], P('ep', 'tp')
- new_keys: bfloat16 [64, 16, 128], P('ep', 'tp')
- new_values: bfloat16 [64, 16, 128], P('ep', 'tp')
- new_gates: float32 [64, 16], P('ep', 'tp')
The draws below stay inside these ranges and needn't reach their ends.
Inputs may be any that keep to these rules, and one draw needn't show every extreme that they name: `group_ids`: within the 16 sequences of each index of ep (aligned blocks of rows), no group is named by more than 8 sequences, a bound that some block reaches. `inner_ids`: each row names 2 different experts of its group. `gate_totals`: along positions the values of each sequence and head never rise.
All inputs are finite; a program needn't handle non-finite values.
Results may differ from the reference program's by a relative error of at most 0.011.
Values may be sent and summed in bfloat16 or wider, within the bound.
No kernel may reach another device: no remote copies, remote signals or barrier semaphores. Data moves between devices by JAX's collectives and lax.ppermute only.
A program may use at most 64 MiB of HBM per device.

```python
import math
import jax
import jax.numpy as jnp
import numpy as np
from jax import lax

D = 2048
HEADS = 16
HEAD_DIM = 128
FFE = 512
EPG = 4
TOPK = 2
FFD = 2048
SEQ_GRP = 16
STORED_ENTRIES = 1024
STREAM_COUNT = 64
GROUPS = 4
CAP = 8
N_EP = 4


def draw_key_cache(key, part):
    full_shape = (STREAM_COUNT, HEADS, STORED_ENTRIES, HEAD_DIM)
    base_draw = jnp.clip(jax.random.normal(jax.random.fold_in(key, 11), full_shape, jnp.float32), -5.0, 5.0)
    return base_draw.astype(jnp.bfloat16)


def draw_gate_totals(key, part):
    noise_child_seeds = jax.random.split(jax.random.fold_in(key, 21), 7)
    slow_share = 0.5
    gradual_zone_flags = jax.random.uniform(noise_child_seeds[0], (1, HEADS, 1), jnp.float32) < slow_share
    slow_total = jax.random.uniform(noise_child_seeds[1], (STREAM_COUNT, HEADS, 1), jnp.float32, 0.2, 0.7)
    fast_span = jax.random.uniform(noise_child_seeds[2], (1, HEADS, 1), jnp.float32, 30.0, 100.0)
    seq_factor = jnp.exp(jax.random.uniform(noise_child_seeds[3], (STREAM_COUNT, 1, 1), jnp.float32, 0.0, math.log(2.0)))
    rough_mult = jax.random.uniform(noise_child_seeds[4], (STREAM_COUNT, HEADS, STORED_ENTRIES), jnp.float32, 0.5, 1.5)
    fading_per_tick = jnp.where(gradual_zone_flags, slow_total / STORED_ENTRIES, 1.0 / fast_span) * seq_factor * rough_mult
    spike_index_point = jax.random.randint(noise_child_seeds[5], (STREAM_COUNT, 1, 1, 2), 0, STORED_ENTRIES)
    entry_indices = jnp.arange(STORED_ENTRIES)[None, None, :, None]
    spike_zone_flags = jnp.any(entry_indices == spike_index_point, axis=-1)
    keeping_logarithm_multiplier = jnp.log(jax.random.uniform(noise_child_seeds[6], (STREAM_COUNT, HEADS, 1), jnp.float32, 0.55, 0.8))
    logarithm_fading_tick = -fading_per_tick + jnp.where(spike_zone_flags & gradual_zone_flags, keeping_logarithm_multiplier, 0.0)
    return jnp.cumsum(logarithm_fading_tick, axis=-1)


def set_ends(array, rng, low, top_value):
    extent = array.shape
    index_at = [jax.random.randint(jax.random.fold_in(rng, axis), (), 0, extent[axis]) for axis in range(len(extent))]
    array = array.at[tuple(index_at)].set(low)
    longest = extent.index(max(extent))
    index_at[longest] = (index_at[longest] + 1) % extent[longest]
    return array.at[tuple(index_at)].set(top_value)


def strengthened(entries, stream_key, source, target, parts, factor):
    def block_of(dim):
        return (jnp.arange(entries.shape[dim]) // (entries.shape[dim] // parts)).reshape((-1,) + (1,) * (entries.ndim - 1 - dim))

    one_side = jax.random.permutation(stream_key, parts)[block_of(target)]
    other_side = (block_of(target) + parts // 2) % parts
    return jnp.where((block_of(source) == one_side) | (block_of(source) == other_side), factor * entries, entries)


def level_of(rng, dims, cuts, least, high):
    loudness = 1.0
    for axis_at, parts in cuts:
        steps = jax.random.uniform(jax.random.fold_in(jax.random.fold_in(rng, 6), axis_at), (parts,), jnp.float32, least / len(cuts), high / len(cuts))
        loudness = loudness * jnp.repeat(jnp.exp(steps), dims[axis_at] // parts).reshape((-1,) + (1,) * (len(dims) - 1 - axis_at))
    return loudness


def choose_distinct(rng, rows, number_of, top, lift):
    sequence = jax.random.permutation(jax.random.fold_in(rng, 1), number_of)
    pull = sequence
    for power in range(3):
        pull = pull * pull // number_of
    pull = pull * lift // number_of
    lots = jax.random.randint(jax.random.fold_in(rng, 2), (rows, number_of), 0, 4096) + pull
    sure = jax.random.permutation(jax.random.fold_in(rng, 3), rows)[jnp.arange(number_of) % rows]
    lots = jnp.where(jnp.arange(rows)[:, None] == sure[None, :], 1 << 14, lots)
    score = lots * number_of + jnp.arange(number_of)
    return lax.top_k(score.astype(jnp.int32), top)[1].astype(jnp.int32)


def shared_out(rng, own, number, rows, number_of, top, bound, lean):
    sequence = jax.random.permutation(rng, number_of)
    crowded, common = portions_of(number_of, rows * top, bound, lean, True), portions_of(number_of, rows * top, bound, lean, False)
    places = jnp.arange(number_of)

    def named(sizes, rotation):
        used = int((sizes > 0).sum())
        fixed = max(1, used // 4)
        shifted = fixed + (places - fixed + rotation * (used - fixed)) % max(1, number_of - fixed)
        return jnp.zeros((number_of,), jnp.int32).at[sequence[jnp.where(places < fixed, places, shifted)]].set(jnp.asarray(sizes, jnp.int32))

    sizes = jnp.where(number % 4 == 0, named(crowded, number // 4), named(common, number - number // 4 - 1))
    mixed = jax.random.permutation(jax.random.fold_in(own, 3), number_of)
    donor, sink = mixed[0:number_of // 2 * 2:2], mixed[1:number_of // 2 * 2:2]
    margin = jnp.minimum(sizes[donor] - 1, bound - sizes[sink]) // 2
    margin = jnp.where((donor == sequence[0]) | (sink == sequence[0]) | (sizes[sink] == 0), 0, jnp.maximum(margin, 0))
    shifted = jax.random.randint(jax.random.fold_in(own, 4), (number_of // 2,), 0, 1 << 20) % (margin + 1)
    sizes = sizes.at[donor].add(-shifted).at[sink].add(shifted)
    items = jnp.searchsorted(jnp.cumsum(sizes), jnp.arange(rows * top), side="right").astype(jnp.int32)
    listing = items.reshape(top, rows).T
    listing = listing[jax.random.permutation(jax.random.fold_in(own, 1), rows)]
    rotation = jax.random.randint(jax.random.fold_in(own, 2), (rows, 1), 0, top)
    return jnp.take_along_axis(listing, (jnp.arange(top)[None, :] + rotation) % top, axis=1)


def portions_of(number_of, total, limit, slope, full):
    weights = [(1 << 20) // math.isqrt(standing ** slope) + 1 for standing in range(1, number_of + 1)]
    largest = limit if full else min(limit, max(-(-total // number_of), total * weights[0] // sum(weights)))
    least = 1 if total - largest >= number_of - 1 else 0
    given, spare = [largest] + [least] * (number_of - 1), total - largest - least * (number_of - 1)
    while spare > 0:
        candidates = [i for i in range(1, number_of) if given[i] < largest] or [i for i in range(1, number_of) if given[i] < limit]
        mass, left = sum([weights[i] for i in candidates]), spare
        for i in candidates:
            addition = min(limit - given[i], max(1, left * weights[i] // mass), spare)
            given[i] = given[i] + addition
            spare = spare - addition
    return np.array(given)


def noise(own_key, shape, deviation, bound, cuts=(), kind=jnp.bfloat16):
    loudness = level_of(own_key, shape, cuts, -0.22, 0.18) if cuts else 1.0
    values = jax.random.normal(own_key, shape, jnp.float32) * deviation * loudness
    return jnp.minimum(jnp.maximum(values, -bound), bound).astype(kind)


def noise_with(stream_key, dims, scale, bound, cuts, heavy, kind=jnp.bfloat16):
    values = scale * jax.random.normal(stream_key, dims, jnp.float32)
    if cuts:
        values = values * level_of(stream_key, dims, cuts, -0.22, 0.18)
    return jnp.clip(strengthened(values, jax.random.fold_in(stream_key, 3), *heavy), -bound, bound).astype(kind)


def setup_inputs(seed: int = 0) -> dict:
    key_list = jax.random.split(jax.random.key(seed), 24)
    tokens = noise(key_list[0], (STREAM_COUNT, D), 1.0, 6.0, ((0, 4), (1, 8)))
    key_cache = draw_key_cache(jax.random.fold_in(key_list[23], 71), 0)
    value_cache = noise(key_list[2], (STREAM_COUNT, HEADS, STORED_ENTRIES, HEAD_DIM), 1.0, 6.0, ((0, 4), (1, 8)))
    gate_totals = draw_gate_totals(jax.random.fold_in(key_list[23], 71), 0)
    lengths = set_ends(jax.random.randint(key_list[4], (STREAM_COUNT,), STORED_ENTRIES // 8, STORED_ENTRIES + 1), jax.random.fold_in(key_list[4], 1), STORED_ENTRIES // 8, STORED_ENTRIES).astype(jnp.int32)
    attn_gain = jnp.clip(1.0 + 0.18 * jax.random.normal(key_list[5], (D,), jnp.float32), 0.1, 1.9)
    w_query = noise(key_list[6], (D, HEADS * HEAD_DIM), D ** -0.5, 0.125, ((1, 8),))
    w_key = noise(key_list[7], (D, HEADS * HEAD_DIM), D ** -0.5, 0.125, ((1, 8),))
    w_value = noise(key_list[8], (D, HEADS * HEAD_DIM), D ** -0.5, 0.125, ((1, 8),))
    w_forget = noise(key_list[9], (D, HEADS), D ** -0.5, 0.125)
    forget_bias = jnp.clip(jax.random.uniform(key_list[10], (HEADS,), jnp.float32, -3.0, 0.0), -3.0, 0.0)
    w_attn_out = noise_with(key_list[11], (HEADS * HEAD_DIM, D), (HEADS * HEAD_DIM) ** -0.5, 0.1875, ((0, 8),), (0, 1, 8, 2.0))
    moe_gain = jnp.clip(1.0 + 0.18 * jax.random.normal(key_list[12], (D,), jnp.float32), 0.1, 1.9)
    group_ids_keys = jax.random.split(jax.random.fold_in(key_list[13], 1), STREAM_COUNT // SEQ_GRP)
    group_ids_turns = jax.random.permutation(jax.random.fold_in(key_list[13], 3), STREAM_COUNT // SEQ_GRP)
    group_ids = jax.vmap(lambda own, number: shared_out(jax.random.fold_in(key_list[13], 2), own, number, SEQ_GRP, N_EP, 1, CAP, 1))(group_ids_keys, group_ids_turns).reshape((STREAM_COUNT, 1))
    inner_ids = choose_distinct(key_list[14], STREAM_COUNT, EPG, TOPK, 0)
    group_prob = jnp.clip(0.2 + 0.8 * jax.random.uniform(key_list[15], (STREAM_COUNT,), jnp.float32) ** level_of(key_list[15], (STREAM_COUNT,), ((0, 4),), -0.2, 0.2), 0.2, 1.0)
    pair_logits = noise(key_list[16], (STREAM_COUNT, TOPK), 1.5, 6.0, ((0, 4),), jnp.float32)
    w_expert_gate = noise(key_list[17], (GROUPS, D, EPG * FFE), D ** -0.5, 0.125, ((0, 4), (2, 8)))
    w_expert_up = noise(key_list[18], (GROUPS, D, EPG * FFE), D ** -0.5, 0.125, ((0, 4), (2, 8)))
    w_expert_down = noise_with(key_list[19], (GROUPS, EPG * FFE, D), FFE ** -0.5, 0.375, ((0, 4), (1, 8)), (1, 2, 8, 2.0))
    w_dense_in = noise(key_list[20], (D, FFD), D ** -0.5, 0.125, ((1, 8),))
    w_dense_out = noise_with(key_list[21], (FFD, D), FFD ** -0.5, 0.1875, ((0, 8),), (0, 1, 8, 2.0))
    dense_gate = jnp.clip(jax.random.uniform(key_list[22], (D,), jnp.float32, -2.0, 2.0) * level_of(key_list[22], (D,), ((0, 8),), -0.4, 0.0), -2.0, 2.0)
    return {"tokens": tokens, "key_cache": key_cache, "value_cache": value_cache, "gate_totals": gate_totals, "lengths": lengths, "attn_gain": attn_gain, "w_query": w_query, "w_key": w_key, "w_value": w_value, "w_forget": w_forget, "forget_bias": forget_bias, "w_attn_out": w_attn_out, "moe_gain": moe_gain, "group_ids": group_ids, "inner_ids": inner_ids, "group_prob": group_prob, "pair_logits": pair_logits, "w_expert_gate": w_expert_gate, "w_expert_up": w_expert_up, "w_expert_down": w_expert_down, "w_dense_in": w_dense_in, "w_dense_out": w_dense_out, "dense_gate": dense_gate}


EPS = 1e-06
FLOOR = -1e+30

def norm_rows(row_data, gain_vec):
    values = row_data.astype(jnp.float32)
    factor = lax.rsqrt(lax.optimization_barrier(jnp.mean(values * values, axis=-1, keepdims=True)) + EPS)
    return (values * factor * gain_vec).astype(jnp.bfloat16)

def head_norm(values):
    factor = lax.rsqrt(lax.optimization_barrier(jnp.mean(values * values, axis=-1, keepdims=True)) + EPS)
    return (values * factor).astype(jnp.bfloat16)

def attend_one(packed):
    queries, fresh_key, fresh_value, key_rows, value_rows, totals, length, current = packed
    score_scale = HEAD_DIM ** (-0.5)
    scores = jnp.einsum('hd,hld->hl', queries.astype(jnp.float32), key_rows.astype(jnp.float32)) * score_scale
    scores = scores + current[:, None] - totals
    entry_indices = jnp.arange(STORED_ENTRIES)
    live_mask = (entry_indices < length)[None, :]
    scores = jnp.where(live_mask, scores, FLOOR)
    own_score = lax.optimization_barrier(jnp.sum(queries.astype(jnp.float32) * fresh_key.astype(jnp.float32), axis=-1)) * score_scale
    peak = jnp.maximum(lax.optimization_barrier(jnp.max(scores, axis=-1)), own_score)
    expo_terms = jnp.where(live_mask, jnp.exp(scores - peak[:, None]), 0.0)
    own_expo = jnp.exp(own_score - peak)
    denom_sum = lax.optimization_barrier(jnp.sum(expo_terms, axis=-1)) + own_expo
    weights = (expo_terms / denom_sum[:, None]).astype(jnp.bfloat16)
    own_weight = (own_expo / denom_sum).astype(jnp.bfloat16)
    attended = jnp.einsum('hl,hld->hd', weights.astype(jnp.float32), value_rows.astype(jnp.float32))
    attended = attended + own_weight.astype(jnp.float32)[:, None] * fresh_value.astype(jnp.float32)
    return attended.astype(jnp.bfloat16)

def reference(tokens, key_cache, value_cache, gate_totals, lengths, attn_gain, w_query, w_key, w_value, w_forget, forget_bias, w_attn_out, moe_gain, group_ids, inner_ids, group_prob, pair_logits, w_expert_gate, w_expert_up, w_expert_down, w_dense_in, w_dense_out, dense_gate):
    normed = norm_rows(tokens, attn_gain)
    seq_count = tokens.shape[0]

    def project(weight):
        return jnp.dot(normed, weight, preferred_element_type=jnp.float32).reshape(seq_count, HEADS, HEAD_DIM)
    queries = head_norm(project(w_query))
    new_keys = head_norm(project(w_key))
    new_values = project(w_value).astype(jnp.bfloat16)
    log_gate = jax.nn.log_sigmoid(jnp.dot(normed, w_forget, preferred_element_type=jnp.float32) + forget_bias)
    last_index = jnp.broadcast_to((lengths - 1).astype(jnp.int32)[:, None, None], (seq_count, HEADS, 1))
    last_total = jnp.take_along_axis(gate_totals, last_index, axis=2)[:, :, 0]
    new_gates = last_total + log_gate
    attended = lax.map(attend_one, (queries, new_keys, new_values, key_cache, value_cache, gate_totals, lengths, new_gates))
    projected = jnp.dot(attended.reshape(seq_count, HEADS * HEAD_DIM), w_attn_out, preferred_element_type=jnp.float32)
    residual = (tokens.astype(jnp.float32) + projected).astype(jnp.bfloat16)
    moe_in = norm_rows(residual, moe_gain)
    first_share = jax.nn.sigmoid(pair_logits[:, 0] - pair_logits[:, 1])
    pair_share = group_prob[:, None] * jnp.stack([first_share, 1.0 - first_share], axis=1)
    pair_share = lax.optimization_barrier(pair_share.astype(jnp.bfloat16)).astype(jnp.float32)
    inner_range = jnp.arange(EPG)
    spread = lax.optimization_barrier(jnp.sum(jnp.where(inner_ids[:, :, None] == inner_range[None, None, :], pair_share[:, :, None], 0.0), axis=1))

    def expert_one(packed):
        token_row, group_id, share_vec = packed
        gate_pre = jnp.dot(token_row[None, :], w_expert_gate[group_id], preferred_element_type=jnp.float32)[0]
        up_pre = jnp.dot(token_row[None, :], w_expert_up[group_id], preferred_element_type=jnp.float32)[0]
        weight_cols = jnp.repeat(share_vec, FFE)
        hidden = (jax.nn.silu(gate_pre) * up_pre * weight_cols).astype(jnp.bfloat16)
        return jnp.dot(hidden[None, :], w_expert_down[group_id], preferred_element_type=jnp.float32)[0].astype(jnp.bfloat16)
    expert_out = lax.map(expert_one, (moe_in, group_ids[:, 0], spread))
    dense_hidden = jax.nn.silu(jnp.dot(moe_in, w_dense_in, preferred_element_type=jnp.float32)).astype(jnp.bfloat16)
    dense_out = jnp.dot(dense_hidden, w_dense_out, preferred_element_type=jnp.float32)
    layer_output = residual.astype(jnp.float32) + expert_out.astype(jnp.float32) + jax.nn.sigmoid(dense_gate) * dense_out
    return (layer_output.astype(jnp.bfloat16), new_keys, new_values, new_gates)
```

```python
import jax
import jax.numpy as jnp
from jax import lax
from jax.sharding import PartitionSpec as P

FFE = 512
EPG = 4


EPS = 1e-06
FLOOR = -1e30


def norm_rows(row_data, gain_vec):
    values = row_data.astype(jnp.float32)
    factor = lax.rsqrt(jnp.mean(values * values, axis=-1, keepdims=True) + EPS)
    return (values * factor * gain_vec).astype(jnp.bfloat16)


def head_norm(values):
    factor = lax.rsqrt(jnp.mean(values * values, axis=-1, keepdims=True) + EPS)
    return (values * factor).astype(jnp.bfloat16)


def attend(queries, fresh_key, fresh_value, key_cache, value_cache, gate_totals, lengths, current):
    score_scale = queries.shape[-1] ** (-0.5)
    scores = (
        jnp.einsum("shd,shld->shl", queries, key_cache, preferred_element_type=jnp.float32)
        * score_scale
    )
    scores = scores + current[:, :, None] - gate_totals
    entry_indices = jnp.arange(key_cache.shape[2])
    live_mask = (entry_indices[None, :] < lengths[:, None])[:, None, :]
    scores = jnp.where(live_mask, scores, FLOOR)
    own_score = (
        jnp.sum(queries.astype(jnp.float32) * fresh_key.astype(jnp.float32), axis=-1) * score_scale
    )
    peak = jnp.maximum(jnp.max(scores, axis=-1), own_score)
    expo_terms = jnp.where(live_mask, jnp.exp(scores - peak[:, :, None]), 0.0)
    own_expo = jnp.exp(own_score - peak)
    denom_sum = jnp.sum(expo_terms, axis=-1) + own_expo
    weights = (expo_terms / denom_sum[:, :, None]).astype(jnp.bfloat16)
    own_weight = (own_expo / denom_sum).astype(jnp.bfloat16)
    attended = jnp.einsum("shl,shld->shd", weights, value_cache, preferred_element_type=jnp.float32)
    attended = attended + own_weight.astype(jnp.float32)[:, :, None] * fresh_value.astype(
        jnp.float32
    )
    return attended.astype(jnp.bfloat16)


def body(
    tokens,
    key_cache,
    value_cache,
    gate_totals,
    lengths,
    attn_gain,
    w_query,
    w_key,
    w_value,
    w_forget,
    forget_bias,
    w_attn_out,
    moe_gain,
    group_ids,
    inner_ids,
    group_prob,
    pair_logits,
    w_expert_gate,
    w_expert_up,
    w_expert_down,
    w_dense_in,
    w_dense_out,
    dense_gate,
):
    tp_size = lax.axis_size("tp")
    groups = lax.axis_size("ep")
    seq_count, width = tokens.shape
    model_dim = width * tp_size
    heads_dev = key_cache.shape[1]
    head_dim = key_cache.shape[3]

    gate_high = lax.reduce_precision(dense_gate, 8, 7)
    gate_low = dense_gate - gate_high
    gate_rows = jnp.pad(jnp.stack([gate_high, gate_low]), ((0, 6), (0, 0))).astype(jnp.bfloat16)
    own_block = jnp.concatenate([tokens, gate_rows], axis=0)
    first_recv = lax.all_to_all(
        jnp.broadcast_to(own_block, (tp_size,) + own_block.shape),
        "tp",
        split_axis=0,
        concat_axis=0,
        tiled=True,
    )
    gathered = first_recv[:, :seq_count].transpose(1, 0, 2).reshape(seq_count, model_dim)
    full_gate = (
        first_recv[:, seq_count].astype(jnp.float32)
        + first_recv[:, seq_count + 1].astype(jnp.float32)
    ).reshape(model_dim)
    normed = norm_rows(gathered, attn_gain)

    def project(weight):
        return jnp.dot(normed, weight, preferred_element_type=jnp.float32).reshape(
            seq_count, heads_dev, head_dim
        )

    queries = head_norm(project(w_query))
    new_keys = head_norm(project(w_key))
    new_values = project(w_value).astype(jnp.bfloat16)
    first_head = lax.axis_index("tp") * heads_dev
    forget_all = jnp.dot(normed, w_forget, preferred_element_type=jnp.float32) + forget_bias
    log_gate = jax.nn.log_sigmoid(lax.dynamic_slice_in_dim(forget_all, first_head, heads_dev, 1))
    entry_indices = jnp.arange(gate_totals.shape[2])
    at_last = (entry_indices[None, :] == (lengths - 1)[:, None])[:, None, :]
    new_gates = jnp.sum(jnp.where(at_last, gate_totals, 0.0), axis=2) + log_gate
    attended = attend(
        queries, new_keys, new_values, key_cache, value_cache, gate_totals, lengths, new_gates
    )
    partial_value = jnp.dot(
        attended.reshape(seq_count, heads_dev * head_dim),
        w_attn_out,
        preferred_element_type=jnp.float32,
    ).astype(jnp.bfloat16)
    pieces = lax.all_to_all(
        partial_value.reshape(seq_count, tp_size, width).transpose(1, 0, 2),
        "tp",
        split_axis=0,
        concat_axis=0,
        tiled=True,
    )
    piece_sum = jnp.sum(pieces.astype(jnp.float32), axis=0)
    own_residual = (tokens.astype(jnp.float32) + piece_sum).astype(jnp.bfloat16)

    capacity = max(2, 2 * seq_count // groups)
    first_share = jax.nn.sigmoid(pair_logits[:, 0] - pair_logits[:, 1])
    pair_share = group_prob[:, None] * jnp.stack([first_share, 1.0 - first_share], axis=1)
    inner_range = jnp.arange(EPG)
    spread = jnp.sum(
        jnp.where(inner_ids[:, :, None] == inner_range[None, None, :], pair_share[:, :, None], 0.0),
        axis=1,
    ).astype(jnp.bfloat16)
    choose = (group_ids == jnp.arange(groups)[None, :]).astype(jnp.int32)
    before = jnp.cumsum(choose, axis=0) - choose
    slot_of = group_ids[:, 0] * capacity + jnp.sum(before * choose, axis=1)
    slot_ids = jnp.arange(groups * capacity)
    send_map = (slot_of[None, :] == slot_ids[:, None]).astype(jnp.bfloat16)
    row_data = jnp.concatenate([own_residual, jnp.pad(spread, ((0, 0), (0, 128 - EPG)))], axis=1)
    send_rows = jnp.dot(send_map, row_data, preferred_element_type=jnp.float32).astype(jnp.bfloat16)
    wide = row_data.shape[1]
    send_blocks = jnp.broadcast_to(
        send_rows.reshape(groups, 1, capacity, wide), (groups, tp_size, capacity, wide)
    ).reshape(groups * tp_size, capacity, wide)
    recv_blocks = lax.all_to_all(
        send_blocks, ("ep", "tp"), split_axis=0, concat_axis=0, tiled=True
    ).reshape(groups, tp_size, capacity, wide)
    recv_rows = (
        recv_blocks[..., :width].transpose(0, 2, 1, 3).reshape(groups * capacity, model_dim)
    )
    recv_weights = recv_blocks[:, 0, :, width : width + EPG].reshape(groups * capacity, EPG)
    moe_in = norm_rows(recv_rows, moe_gain)
    hidden_dev = w_expert_gate.shape[2]
    expert_index = lax.axis_index("tp") * hidden_dev // FFE
    route_col = jnp.sum(
        jnp.where(inner_range[None, :] == expert_index, recv_weights.astype(jnp.float32), 0.0),
        axis=1,
    )
    dense_hidden = jax.nn.silu(
        jnp.dot(moe_in, w_dense_in, preferred_element_type=jnp.float32)
    ).astype(jnp.bfloat16)
    gate_pre = jnp.dot(moe_in, w_expert_gate[0], preferred_element_type=jnp.float32)
    up_pre = jnp.dot(moe_in, w_expert_up[0], preferred_element_type=jnp.float32)
    hidden = (jax.nn.silu(gate_pre) * up_pre * route_col[:, None]).astype(jnp.bfloat16)
    dense_part = jnp.dot(dense_hidden, w_dense_out, preferred_element_type=jnp.float32)
    expert_part = jnp.dot(hidden, w_expert_down[0], preferred_element_type=jnp.float32)
    both = (expert_part + jax.nn.sigmoid(full_gate) * dense_part).astype(jnp.bfloat16)
    returned = lax.all_to_all(
        both.reshape(groups, capacity, tp_size, width)
        .transpose(0, 2, 1, 3)
        .reshape(groups * tp_size, capacity, width),
        ("ep", "tp"),
        split_axis=0,
        concat_axis=0,
        tiled=True,
    ).reshape(groups * tp_size * capacity, width)
    take_map = jnp.broadcast_to(
        send_map.reshape(groups, 1, capacity, seq_count),
        (groups, tp_size, capacity, seq_count),
    ).reshape(groups * tp_size * capacity, seq_count)
    branch_sum = lax.dot_general(
        take_map, returned, (((0,), (0,)), ((), ())), preferred_element_type=jnp.float32
    )
    layer_output = own_residual.astype(jnp.float32) + branch_sum
    return (layer_output.astype(jnp.bfloat16), new_keys, new_values, new_gates)


def solution(mesh):
    placed = (
        P("ep", "tp"),
        P("ep", "tp", None, None),
        P("ep", "tp", None, None),
        P("ep", "tp", None),
        P("ep"),
        P(),
        P(None, "tp"),
        P(None, "tp"),
        P(None, "tp"),
        P(),
        P(),
        P("tp", None),
        P(),
        P("ep", None),
        P("ep", None),
        P("ep"),
        P("ep", None),
        P("ep", None, "tp"),
        P("ep", None, "tp"),
        P("ep", "tp", None),
        P(None, "tp"),
        P("tp", None),
        P("tp"),
    )
    return jax.shard_map(
        body,
        mesh=mesh,
        in_specs=placed,
        out_specs=(P("ep", "tp"), P("ep", "tp", None), P("ep", "tp", None), P("ep", "tp")),
        check_vma=False,
    )
```

```python
import jax
import jax.numpy as jnp
from jax import lax
from jax.experimental import pallas as pl
from jax.experimental.pallas import tpu as pltpu
from jax.sharding import PartitionSpec as P

FFE = 512
EPG = 4


EPS = 1e-06
FLOOR = -1e30


def norm_rows(row_data, gain_vec):
    values = row_data.astype(jnp.float32)
    factor = lax.rsqrt(jnp.mean(values * values, axis=-1, keepdims=True) + EPS)
    return (values * factor * gain_vec).astype(jnp.bfloat16)


def head_norm(values):
    factor = lax.rsqrt(jnp.mean(values * values, axis=-1, keepdims=True) + EPS)
    return (values * factor).astype(jnp.bfloat16)


def pack_kernel(tokens_ref, gate_ref, out_ref):
    copies, _, width = out_ref.shape
    rows = tokens_ref.shape[0]
    gate = gate_ref[...]
    high = gate.astype(jnp.bfloat16)
    low = (gate - high.astype(jnp.float32)).astype(jnp.bfloat16)
    index = lax.broadcasted_iota(jnp.int32, (8, width), 0)
    extra = jnp.where(
        index == 0, high.astype(jnp.float32), jnp.where(index == 1, low.astype(jnp.float32), 0.0)
    ).astype(jnp.bfloat16)
    tokens = tokens_ref[...]
    for copy in range(copies):
        out_ref[copy, :rows] = tokens
        out_ref[copy, rows:] = extra


def attend_kernel(
    len_smem,
    first_smem,
    x_ref,
    gain_ref,
    len_ref,
    totals_ref,
    wf_ref,
    bias_ref,
    wq_hbm,
    wk_hbm,
    wv_hbm,
    key_hbm,
    value_hbm,
    wo_hbm,
    out_ref,
    new_key_ref,
    new_value_ref,
    new_gate_ref,
    wq,
    wk,
    wv,
    wo,
    keys,
    values,
    score_ref,
    weight_sem,
    key_sem,
    value_sem,
):
    seqs, heads, entries, dim = keys.shape
    chunk = min(256, entries)
    chunks = entries // chunk
    weight_copies = [
        pltpu.make_async_copy(src, dst, weight_sem.at[n])
        for n, (src, dst) in enumerate(
            ((wq_hbm, wq), (wk_hbm, wk), (wv_hbm, wv), (wo_hbm, wo))
        )
    ]

    def cache_copy(src, dst, sem, seq, part):
        cut = pl.ds(0, (part + 1) * chunk)
        return pltpu.make_async_copy(src.at[seq, :, cut, :], dst.at[seq, :, cut, :], sem.at[seq])

    def for_live(action):
        for seq in range(seqs):
            last_part = (len_smem[seq] - 1) // chunk
            for part in range(chunks):
                pl.when(last_part == part)(lambda: action(seq, part))

    for copy in weight_copies[:3]:
        copy.start()
    for_live(lambda seq, part: cache_copy(key_hbm, keys, key_sem, seq, part).start())

    x = x_ref[...].astype(jnp.float32)
    factor = lax.rsqrt(jnp.mean(x * x, axis=-1, keepdims=True) + EPS)
    normed = (x * factor * gain_ref[...]).astype(jnp.bfloat16)
    forget = jnp.dot(normed, wf_ref[...], preferred_element_type=jnp.float32) + bias_ref[...]
    lane = lax.broadcasted_iota(jnp.int32, forget.shape, 1)
    forget_col = jnp.concatenate(
        [
            jnp.sum(jnp.where(lane == first_smem[0] + h, forget, 0.0), axis=1, keepdims=True)
            for h in range(heads)
        ],
        axis=0,
    )
    log_gate = jnp.minimum(forget_col, 0.0) - jnp.log1p(jnp.exp(-jnp.abs(forget_col)))
    totals = totals_ref[...]
    place = lax.broadcasted_iota(jnp.int32, totals.shape, 1)
    length_col = jnp.concatenate([len_ref[...]] * heads, axis=0)
    current = (
        jnp.sum(jnp.where(place == length_col - 1, totals, 0.0), axis=1, keepdims=True) + log_gate
    )
    new_gate_ref[...] = jnp.concatenate(
        [current[h * seqs : (h + 1) * seqs] for h in range(heads)], axis=1
    )
    for seq in range(seqs):
        for part in range(1, chunks):

            @pl.when(part * chunk >= len_smem[seq])
            def _():
                values[seq, :, part * chunk : (part + 1) * chunk, :] = jnp.zeros(
                    (heads, chunk, dim), values.dtype
                )

    def project(n, weight):
        weight_copies[n].wait()
        return jnp.dot(normed, weight[...], preferred_element_type=jnp.float32)

    def head_rows(z):
        return [z[:, h * dim : (h + 1) * dim] for h in range(heads)]

    query_rows = [head_norm(z) for z in head_rows(project(0, wq))]
    key_rows = [head_norm(z) for z in head_rows(project(1, wk))]
    value_rows = [z.astype(jnp.bfloat16) for z in head_rows(project(2, wv))]
    new_key_ref[...] = jnp.concatenate(key_rows, axis=1)
    new_value_ref[...] = jnp.concatenate(value_rows, axis=1)
    for_live(lambda seq, part: cache_copy(value_hbm, values, value_sem, seq, part).start())
    weight_copies[3].start()
    for_live(lambda seq, part: cache_copy(key_hbm, keys, key_sem, seq, part).wait())
    for seq in range(seqs):
        for h in range(heads):
            raw = lax.dot_general(
                query_rows[h],
                keys[seq, h],
                (((1,), (1,)), ((), ())),
                preferred_element_type=jnp.float32,
            )
            score_ref[h * seqs + seq : h * seqs + seq + 1, :] = raw[seq : seq + 1, :]
    scale = dim ** (-0.5)
    live = place < length_col
    scores = jnp.where(live, score_ref[...] * scale + current - totals, FLOOR)
    own_score = (
        jnp.concatenate(
            [
                jnp.sum(q.astype(jnp.float32) * k.astype(jnp.float32), axis=1, keepdims=True)
                for q, k in zip(query_rows, key_rows)
            ],
            axis=0,
        )
        * scale
    )
    peak = jnp.maximum(jnp.max(scores, axis=1, keepdims=True), own_score)
    expo = jnp.where(live, jnp.exp(scores - peak), 0.0)
    own_expo = jnp.exp(own_score - peak)
    denom = jnp.sum(expo, axis=1, keepdims=True) + own_expo
    weights = (expo / denom).astype(jnp.bfloat16)
    own_weight = (own_expo / denom).astype(jnp.bfloat16).astype(jnp.float32)
    for_live(lambda seq, part: cache_copy(value_hbm, values, value_sem, seq, part).wait())
    attended = []
    for h in range(heads):
        head_weights = weights[h * seqs : (h + 1) * seqs]
        for seq in range(seqs):
            mixed = jnp.dot(head_weights, values[seq, h], preferred_element_type=jnp.float32)
            score_ref[h * seqs + seq : h * seqs + seq + 1, :dim] = mixed[seq : seq + 1, :]
        block = slice(h * seqs, (h + 1) * seqs)
        attended.append(
            score_ref[block, :dim] + own_weight[block] * value_rows[h].astype(jnp.float32)
        )
    joined = jnp.concatenate(attended, axis=1).astype(jnp.bfloat16)
    weight_copies[3].wait()
    width = out_ref.shape[2]
    partial = jnp.dot(joined, wo[...], preferred_element_type=jnp.float32).astype(jnp.bfloat16)
    for piece in range(out_ref.shape[0]):
        out_ref[piece] = partial[:, piece * width : (piece + 1) * width]


def branch_kernel(
    expert_smem, recv_ref, gain_ref, gate_ref, wg_hbm, wu_hbm, wi_hbm, wd_hbm, wo_hbm,
    out_ref, wg, wu, wi, wd, wo, rows_ref, route_ref, sems,
):
    copies = [
        pltpu.make_async_copy(src, dst, sems.at[n])
        for n, (src, dst) in enumerate(
            ((wg_hbm.at[0], wg), (wu_hbm.at[0], wu), (wi_hbm, wi), (wd_hbm.at[0], wd), (wo_hbm, wo))
        )
    ]
    for copy in copies:
        copy.start()
    blocks, capacity, wide = recv_ref.shape
    width = wide - 128
    tp_size = rows_ref.shape[1] // width
    for block in range(blocks):
        group, piece = divmod(block, tp_size)
        place = slice(group * capacity, (group + 1) * capacity)
        rows_ref[place, piece * width : (piece + 1) * width] = recv_ref[block, :, :width].astype(
            jnp.float32
        )
        if piece == 0:
            route_ref[place, :] = recv_ref[block, :, width:].astype(jnp.float32)
    lane = lax.broadcasted_iota(jnp.int32, route_ref.shape, 1)
    route = jnp.sum(
        jnp.where(lane == expert_smem[0], route_ref[...], 0.0), axis=1, keepdims=True
    )
    moe_in = norm_rows(rows_ref[...], gain_ref[...])

    def product(n, left, weight):
        copies[n].wait()
        return jnp.dot(left, weight[...], preferred_element_type=jnp.float32)

    gate_pre = product(0, moe_in, wg)
    up_pre = product(1, moe_in, wu)
    hidden = (gate_pre * jax.nn.sigmoid(gate_pre) * up_pre * route).astype(jnp.bfloat16)
    dense_pre = product(2, moe_in, wi)
    dense_hidden = (dense_pre * jax.nn.sigmoid(dense_pre)).astype(jnp.bfloat16)
    expert_part = product(3, hidden, wd)
    dense_part = product(4, dense_hidden, wo)
    both = (expert_part + jax.nn.sigmoid(gate_ref[...]) * dense_part).astype(jnp.bfloat16)
    out_ref[...] = both


def body(
    tokens,
    key_cache,
    value_cache,
    gate_totals,
    lengths,
    attn_gain,
    w_query,
    w_key,
    w_value,
    w_forget,
    forget_bias,
    w_attn_out,
    moe_gain,
    group_ids,
    inner_ids,
    group_prob,
    pair_logits,
    w_expert_gate,
    w_expert_up,
    w_expert_down,
    w_dense_in,
    w_dense_out,
    dense_gate,
):
    tp_size = lax.axis_size("tp")
    groups = lax.axis_size("ep")
    seq_count, width = tokens.shape
    model_dim = width * tp_size
    heads_dev = key_cache.shape[1]
    head_dim = key_cache.shape[3]

    own_block = pl.pallas_call(
        pack_kernel,
        out_shape=jax.ShapeDtypeStruct((tp_size, seq_count + 8, width), jnp.bfloat16),
        name="pack",
    )(tokens, dense_gate[None, :])
    first_recv = lax.all_to_all(
        own_block,
        "tp",
        split_axis=0,
        concat_axis=0,
        tiled=True,
    )
    gathered = first_recv[:, :seq_count].transpose(1, 0, 2).reshape(seq_count, model_dim)
    first_head = lax.axis_index("tp") * heads_dev
    entries = key_cache.shape[2]
    rows = heads_dev * seq_count
    vmem = pl.BlockSpec(memory_space=pltpu.VMEM)
    smem = pl.BlockSpec(memory_space=pltpu.SMEM)
    hbm = pl.BlockSpec(memory_space=pl.ANY)
    blocks_out, new_keys, new_values, new_gates = pl.pallas_call(
        attend_kernel,
        in_specs=[smem, smem] + [vmem] * 6 + [hbm] * 6,
        out_specs=[vmem] * 4,
        out_shape=[
            jax.ShapeDtypeStruct((tp_size, seq_count, width), jnp.bfloat16),
            jax.ShapeDtypeStruct((seq_count, heads_dev * head_dim), jnp.bfloat16),
            jax.ShapeDtypeStruct((seq_count, heads_dev * head_dim), jnp.bfloat16),
            jax.ShapeDtypeStruct((seq_count, heads_dev), jnp.float32),
        ],
        scratch_shapes=[
            pltpu.VMEM(w_query.shape, jnp.bfloat16),
            pltpu.VMEM(w_key.shape, jnp.bfloat16),
            pltpu.VMEM(w_value.shape, jnp.bfloat16),
            pltpu.VMEM(w_attn_out.shape, jnp.bfloat16),
            pltpu.VMEM(key_cache.shape, jnp.bfloat16),
            pltpu.VMEM(value_cache.shape, jnp.bfloat16),
            pltpu.VMEM((rows, entries), jnp.float32),
            pltpu.SemaphoreType.DMA((4,)),
            pltpu.SemaphoreType.DMA((seq_count,)),
            pltpu.SemaphoreType.DMA((seq_count,)),
        ],
        name="attend",
    )(
        lengths,
        first_head.astype(jnp.int32)[None],
        gathered,
        attn_gain[None, :],
        lengths[:, None],
        gate_totals.transpose(1, 0, 2).reshape(rows, entries),
        w_forget,
        forget_bias[None, :],
        w_query,
        w_key,
        w_value,
        key_cache,
        value_cache,
        w_attn_out,
    )
    new_keys = new_keys.reshape(seq_count, heads_dev, head_dim)
    new_values = new_values.reshape(seq_count, heads_dev, head_dim)
    blocks_out, first_recv, group_ids, inner_ids, group_prob, pair_logits = (
        lax.optimization_barrier(
            (blocks_out, first_recv, group_ids, inner_ids, group_prob, pair_logits)
        )
    )
    full_gate = (
        first_recv[:, seq_count].astype(jnp.float32)
        + first_recv[:, seq_count + 1].astype(jnp.float32)
    ).reshape(1, model_dim)
    pieces = lax.all_to_all(
        blocks_out,
        "tp",
        split_axis=0,
        concat_axis=0,
        tiled=True,
    )
    piece_sum = jnp.sum(pieces.astype(jnp.float32), axis=0)
    own_residual = (tokens.astype(jnp.float32) + piece_sum).astype(jnp.bfloat16)

    capacity = max(2, 2 * seq_count // groups)
    first_share = jax.nn.sigmoid(pair_logits[:, 0] - pair_logits[:, 1])
    pair_share = group_prob[:, None] * jnp.stack([first_share, 1.0 - first_share], axis=1)
    inner_range = jnp.arange(EPG)
    spread = jnp.sum(
        jnp.where(inner_ids[:, :, None] == inner_range[None, None, :], pair_share[:, :, None], 0.0),
        axis=1,
    ).astype(jnp.bfloat16)
    choose = (group_ids == jnp.arange(groups)[None, :]).astype(jnp.int32)
    before = jnp.cumsum(choose, axis=0) - choose
    slot_of = group_ids[:, 0] * capacity + jnp.sum(before * choose, axis=1)
    slot_ids = jnp.arange(groups * capacity)
    send_map = (slot_of[None, :] == slot_ids[:, None]).astype(jnp.bfloat16)
    row_data = jnp.concatenate([own_residual, jnp.pad(spread, ((0, 0), (0, 128 - EPG)))], axis=1)
    send_rows = jnp.dot(send_map, row_data, preferred_element_type=jnp.float32).astype(jnp.bfloat16)
    wide = row_data.shape[1]
    send_blocks = jnp.broadcast_to(
        send_rows.reshape(groups, 1, capacity, wide), (groups, tp_size, capacity, wide)
    ).reshape(groups * tp_size, capacity, wide)
    recv_blocks = lax.all_to_all(
        send_blocks, ("ep", "tp"), split_axis=0, concat_axis=0, tiled=True
    )
    expert_index = lax.axis_index("tp") * w_expert_gate.shape[2] // FFE
    both = pl.pallas_call(
        branch_kernel,
        in_specs=[smem] + [vmem] * 3 + [hbm] * 5,
        out_specs=vmem,
        out_shape=jax.ShapeDtypeStruct((groups * capacity, model_dim), jnp.bfloat16),
        scratch_shapes=[
            pltpu.VMEM(w_expert_gate.shape[1:], jnp.bfloat16),
            pltpu.VMEM(w_expert_up.shape[1:], jnp.bfloat16),
            pltpu.VMEM(w_dense_in.shape, jnp.bfloat16),
            pltpu.VMEM(w_expert_down.shape[1:], jnp.bfloat16),
            pltpu.VMEM(w_dense_out.shape, jnp.bfloat16),
            pltpu.VMEM((groups * capacity, model_dim), jnp.float32),
            pltpu.VMEM((groups * capacity, 128), jnp.float32),
            pltpu.SemaphoreType.DMA((5,)),
        ],
        name="branches",
    )(
        expert_index.astype(jnp.int32)[None],
        recv_blocks,
        moe_gain[None, :],
        full_gate,
        w_expert_gate,
        w_expert_up,
        w_dense_in,
        w_expert_down,
        w_dense_out,
    )
    returned = lax.all_to_all(
        both.reshape(groups, capacity, tp_size, width)
        .transpose(0, 2, 1, 3)
        .reshape(groups * tp_size, capacity, width),
        ("ep", "tp"),
        split_axis=0,
        concat_axis=0,
        tiled=True,
    ).reshape(groups * tp_size * capacity, width)
    take_map = jnp.broadcast_to(
        send_map.reshape(groups, 1, capacity, seq_count),
        (groups, tp_size, capacity, seq_count),
    ).reshape(groups * tp_size * capacity, seq_count)
    branch_sum = lax.dot_general(
        take_map, returned, (((0,), (0,)), ((), ())), preferred_element_type=jnp.float32
    )
    layer_output = own_residual.astype(jnp.float32) + branch_sum
    return (layer_output.astype(jnp.bfloat16), new_keys, new_values, new_gates)


def solution(mesh):
    placed = (
        P("ep", "tp"),
        P("ep", "tp", None, None),
        P("ep", "tp", None, None),
        P("ep", "tp", None),
        P("ep"),
        P(),
        P(None, "tp"),
        P(None, "tp"),
        P(None, "tp"),
        P(),
        P(),
        P("tp", None),
        P(),
        P("ep", None),
        P("ep", None),
        P("ep"),
        P("ep", None),
        P("ep", None, "tp"),
        P("ep", None, "tp"),
        P("ep", "tp", None),
        P(None, "tp"),
        P("tp", None),
        P("tp"),
    )
    return jax.shard_map(
        body,
        mesh=mesh,
        in_specs=placed,
        out_specs=(P("ep", "tp"), P("ep", "tp", None), P("ep", "tp", None), P("ep", "tp")),
        check_vma=False,
    )
```
